32 devices in a mesh: gr: 2 (over core), fs: 8 (over z, y), tp: 2 (over x).
Axes of the slice: x: 2, y: 2, z: 4, core: 2. Of those that a mesh axis runs over, the one named last changes fastest.
Arguments:
- tokens: bfloat16 [3072, 2048], P(('gr', 'fs')), may hold values from -6 to 6
- routes: int32 [3072, 8], P(('gr', 'fs')), may hold values from 0 to 15, all different within a row; in each aligned block of 192 rows (0 to 191, 192 to 383, ...) at most 144 rows name the same one
- route_weight: float32 [3072, 8], P(('gr', 'fs')), may hold values from 0.05 to 0.6
- norm_gain: float32 [2048], replicated, may hold values from 0.1 to 1.9
- gate_experts: float32 [2, 8, 512, 2048], P('gr', None, 'fs', 'tp'), may hold values from -0.125 to 0.125
- up_experts: float32 [2, 8, 512, 2048], P('gr', None, 'fs', 'tp'), may hold values from -0.125 to 0.125
- down_experts: float32 [2, 8, 512, 2048], P('gr', None, 'fs', 'tp'), may hold values from -0.25 to 0.25
- gate_shared: float32 [2048, 512], P('fs', 'tp'), may hold values from -0.125 to 0.125
- up_shared: float32 [2048, 512], P('fs', 'tp'), may hold values from -0.125 to 0.125
- down_shared: float32 [512, 2048], P('fs', 'tp'), may hold values from -0.25 to 0.25
Outputs:
- mixed: bfloat16 [3072, 2048], P(('gr', 'fs'), 'tp')
- gate_served: bfloat16 [2, 8, 512, 2048], P(None, 'fs', 'tp')
- up_served: bfloat16 [2, 8, 512, 2048], P(None, 'fs', 'tp')
- down_served: bfloat16 [2, 8, 512, 2048], P(None, 'fs', None, 'tp')
- gate_shared_served: bfloat16 [2048, 512], P(None, 'tp')
- up_shared_served: bfloat16 [2048, 512], P(None, 'tp')
- down_shared_served: bfloat16 [512, 2048], P(None, 'tp')
The draws below stay inside these ranges and needn't reach their ends.
Inputs may be any that keep to these rules, and one draw needn't show every extreme that they name: `routes`: each row names 8 different experts; within the 192 rows of one device no expert is named by more than 144 rows, and some expert reaches 144.
All inputs are finite; a program needn't handle non-finite values.
Results may differ from the reference program's by a relative error of at most 0.0084.
Values may be sent and summed in bfloat16 or wider, within the bound.
A program may use at most 128 MiB of HBM per device.

```python
import math
import jax
import jax.numpy as jnp
import numpy as np
from jax import lax

D = 2048
DE = 512
DS = 512
TOP_K = 8
EXP_HALF = 1
TOK_DEV = 192
EXPERTS = 16
CAP = 144
TOKENS = 3072
N_GR = 2
N_FS = 8


def shard_levels(own_key, shape, pieces, low, largest):
    gain = 1.0
    for dim, shards_of in pieces:
        heights = jax.random.uniform(jax.random.fold_in(jax.random.fold_in(own_key, 6), dim), (shards_of,), jnp.float32, low / len(pieces), largest / len(pieces))
        gain = gain * jnp.repeat(jnp.exp(heights), shape[dim] // shards_of).reshape((-1,) + (1,) * (len(shape) - 1 - dim))
    return gain


def shared_out(stream_key, own, number, rows, number_of, top, most, slope):
    order = jax.random.permutation(stream_key, number_of)
    packed, ordinary = portions_of(number_of, rows * top, most, slope, True), portions_of(number_of, rows * top, most, slope, False)
    places = jnp.arange(number_of)

    def named(lengths, turn):
        used = int((lengths > 0).sum())
        fixed = max(1, used // 4)
        moved = fixed + (places - fixed + turn * (used - fixed)) % max(1, number_of - fixed)
        return jnp.zeros((number_of,), jnp.int32).at[order[jnp.where(places < fixed, places, moved)]].set(jnp.asarray(lengths, jnp.int32))

    lengths = jnp.where(number % 4 == 0, named(packed, number // 4), named(ordinary, number - number // 4 - 1))
    mixed = jax.random.permutation(jax.random.fold_in(own, 3), number_of)
    source_of, sink = mixed[0:number_of // 2 * 2:2], mixed[1:number_of // 2 * 2:2]
    margin = jnp.minimum(lengths[source_of] - 1, most - lengths[sink]) // 2
    margin = jnp.where((source_of == order[0]) | (sink == order[0]) | (lengths[sink] == 0), 0, jnp.maximum(margin, 0))
    moved = jax.random.randint(jax.random.fold_in(own, 4), (number_of // 2,), 0, 1 << 20) % (margin + 1)
    lengths = lengths.at[source_of].add(-moved).at[sink].add(moved)
    items = jnp.searchsorted(jnp.cumsum(lengths), jnp.arange(rows * top), side="right").astype(jnp.int32)
    table = items.reshape(top, rows).T
    table = table[jax.random.permutation(jax.random.fold_in(own, 1), rows)]
    turn = jax.random.randint(jax.random.fold_in(own, 2), (rows, 1), 0, top)
    return jnp.take_along_axis(table, (jnp.arange(top)[None, :] + turn) % top, axis=1)


def portions_of(amount, total, most, skew, full):
    weights = [(1 << 20) // math.isqrt(standing ** skew) + 1 for standing in range(1, amount + 1)]
    largest = most if full else min(most, max(-(-total // amount), total * weights[0] // sum(weights)))
    least = 1 if total - largest >= amount - 1 else 0
    given, surplus = [largest] + [least] * (amount - 1), total - largest - least * (amount - 1)
    while surplus > 0:
        candidates = [i for i in range(1, amount) if given[i] < largest] or [i for i in range(1, amount) if given[i] < most]
        mass, remaining = sum([weights[i] for i in candidates]), surplus
        for i in candidates:
            extra = min(most - given[i], max(1, remaining * weights[i] // mass), surplus)
            given[i] = given[i] + extra
            surplus = surplus - extra
    return np.array(given)


def normal_values(rng, dims, scale, most, pieces=(), kind=jnp.bfloat16):
    entries = scale * jax.random.normal(rng, dims, jnp.float32)
    if pieces:
        entries = entries * shard_levels(rng, dims, pieces, -0.22, 0.18)
    return jnp.clip(entries, -most, most).astype(kind)


def setup_inputs(seed: int = 0) -> dict:
    seeds = jax.random.split(jax.random.key(seed), 11)
    tokens = normal_values(seeds[0], (TOKENS, D), 1.0, 6.0, ((0, 16),))
    routes_keys = jax.random.split(jax.random.fold_in(seeds[1], 1), TOKENS // TOK_DEV)
    routes_turns = jax.random.permutation(jax.random.fold_in(seeds[1], 3), TOKENS // TOK_DEV)
    routes = jax.vmap(lambda own, number: shared_out(jax.random.fold_in(seeds[1], 2), own, number, TOK_DEV, EXPERTS, TOP_K, CAP, 1))(routes_keys, routes_turns).reshape((TOKENS, TOP_K))
    route_weight = jnp.clip(jnp.exp(math.log(0.6) - 2.4849067 * jax.random.uniform(seeds[2], (TOKENS, TOP_K), jnp.float32) ** shard_levels(seeds[2], (TOKENS, TOP_K), ((0, 16),), -0.2, 0.2)), 0.05, 0.6)
    norm_gain = jnp.clip(1.0 + 0.18 * jax.random.normal(seeds[3], (D,), jnp.float32), 0.1, 1.9)
    gate_experts = normal_values(seeds[4], (N_GR, EXP_HALF * N_FS, DE, D), D ** -0.5, 0.125, ((0, 2), (2, 8), (3, 2)), jnp.float32)
    up_experts = normal_values(seeds[5], (N_GR, EXP_HALF * N_FS, DE, D), D ** -0.5, 0.125, ((0, 2), (2, 8), (3, 2)), jnp.float32)
    down_experts = normal_values(seeds[6], (N_GR, EXP_HALF * N_FS, DE, D), DE ** -0.5, 0.25, ((0, 2), (2, 8), (3, 2)), jnp.float32)
    gate_shared = normal_values(seeds[7], (D, DS), D ** -0.5, 0.125, ((0, 8), (1, 2)), jnp.float32)
    up_shared = normal_values(seeds[8], (D, DS), D ** -0.5, 0.125, ((0, 8), (1, 2)), jnp.float32)
    down_shared = normal_values(seeds[9], (DS, D), DS ** -0.5, 0.25, ((0, 8), (1, 2)), jnp.float32)
    return dict(tokens=tokens, routes=routes, route_weight=route_weight, norm_gain=norm_gain, gate_experts=gate_experts, up_experts=up_experts, down_experts=down_experts, gate_shared=gate_shared, up_shared=up_shared, down_shared=down_shared)


EPS = 1e-06

def reference(tokens, routes, route_weight, norm_gain, gate_experts, up_experts, down_experts, gate_shared, up_shared, down_shared):
    bf = jnp.bfloat16
    f32 = jnp.float32
    gate_served = (gate_experts * norm_gain[None, None, None, :]).astype(bf)
    up_served = (up_experts * norm_gain[None, None, None, :]).astype(bf)
    down_served = down_experts.astype(bf)
    gate_sh = (gate_shared * norm_gain[:, None]).astype(bf)
    up_sh = (up_shared * norm_gain[:, None]).astype(bf)
    down_sh = down_shared.astype(bf)
    values = tokens.astype(f32)
    normed = (values * lax.rsqrt(lax.optimization_barrier(jnp.mean(values * values, axis=-1, keepdims=True)) + EPS)).astype(bf)
    count = EXPERTS
    slots_all = CAP * N_GR * N_FS
    flat_e = routes.reshape(-1).astype(jnp.int32)
    assigned = flat_e.shape[0]
    onehot = (flat_e[:, None] == jnp.arange(count, dtype=jnp.int32)[None, :]).astype(jnp.int32)
    ranks = lax.optimization_barrier(jnp.sum(jnp.cumsum(onehot, axis=0) * onehot, axis=1)) - 1
    position = (flat_e * slots_all + ranks).astype(jnp.int32)
    token_of = (jnp.arange(assigned, dtype=jnp.int32) // TOP_K).astype(jnp.int32)
    table = jnp.full((count * slots_all,), TOKENS, jnp.int32).at[position].set(token_of)
    padded = jnp.concatenate([normed, jnp.zeros((1, D), bf)], axis=0)

    def one_expert(args):
        index, w_gate, w_up, w_down = args
        rows = padded[index]
        gate = jnp.dot(rows, w_gate.T, preferred_element_type=f32)
        upper = jnp.dot(rows, w_up.T, preferred_element_type=f32)
        hidden = (jax.nn.silu(gate) * upper).astype(bf)
        return jnp.dot(hidden, w_down, preferred_element_type=f32).astype(bf)
    outputs = lax.map(one_expert, (table.reshape(count, slots_all), gate_served.reshape(count, DE, D), up_served.reshape(count, DE, D), down_served.reshape(count, DE, D)))
    picked = outputs.reshape(count * slots_all, D)[position].reshape(TOKENS, TOP_K, D)
    routed = lax.optimization_barrier(jnp.sum(picked.astype(f32) * route_weight[:, :, None], axis=1))
    shared_hidden = (jax.nn.silu(jnp.dot(normed, gate_sh, preferred_element_type=f32)) * jnp.dot(normed, up_sh, preferred_element_type=f32)).astype(bf)
    shared = jnp.dot(shared_hidden, down_sh, preferred_element_type=f32)
    mixed = (routed + shared).astype(bf)
    return (mixed, gate_served, up_served, down_served, gate_sh, up_sh, down_sh)
```

```python
import jax
import jax.numpy as jnp
from jax import lax
from jax.experimental import pallas as pl
from jax.experimental.pallas import tpu as pltpu
from jax.sharding import PartitionSpec as P

EPS = 1e-06
MESH = pl.DeviceIdType.MESH


def exchange_kernel(dims, g_loc, u_loc, d_loc, g_out, u_out, d_out, send, recv, d_send, d_recv,
                    own, f_send, f_recv, fd_send, fd_recv):
    n_gr, n_fs, n_tp = dims
    gr, fs, tp = lax.axis_index("gr"), lax.axis_index("fs"), lax.axis_index("tp")
    held = g_loc.shape[0] // n_fs
    rows, cols = g_loc.shape[1], g_loc.shape[2]
    per = g_out.shape[2] // rows
    barrier = pltpu.get_barrier_semaphore()

    def greet(i, carry):
        f, t = i // n_tp, i % n_tp

        @pl.when((f != fs) | (t != tp))
        def _():
            pl.semaphore_signal(barrier, inc=1, device_id=(gr, f, t), device_id_type=MESH)
        return carry

    lax.fori_loop(0, n_fs * n_tp, greet, 0)
    for p in range(1, n_gr):
        pl.semaphore_signal(
            barrier, inc=1, device_id=((gr + p) % n_gr, fs, tp), device_id_type=MESH
        )
    pl.semaphore_wait(barrier, n_fs * n_tp - 1 + n_gr - 1)

    to_tp = fs // per
    mine = pl.multiple_of(tp * cols, cols)

    def wide(loc, out, m, d):
        k = (fs + d) % n_fs
        return pltpu.make_async_remote_copy(
            src_ref=loc.at[pl.ds(k * held, held)],
            dst_ref=out.at[gr, :, pl.ds(pl.multiple_of((fs % per) * rows, rows), rows), pl.ds(mine, cols)],
            send_sem=send.at[m, d],
            recv_sem=recv.at[m, fs % per, tp],
            device_id=(gr, k, to_tp),
            device_id_type=MESH,
        )

    def wide_own(loc, out, m):
        return pltpu.make_async_copy(
            loc.at[pl.ds(fs * held, held)],
            out.at[gr, :, pl.ds(pl.multiple_of((fs % per) * rows, rows), rows), pl.ds(mine, cols)],
            own.at[m],
        )

    def tall(d):
        k = (fs + d) % n_fs
        return pltpu.make_async_remote_copy(
            src_ref=d_loc.at[pl.ds(k * held, held)],
            dst_ref=d_out.at[gr, :, pl.ds(pl.multiple_of(fs * rows, rows), rows), :],
            send_sem=d_send.at[d],
            recv_sem=d_recv.at[fs],
            device_id=(gr, k, tp),
            device_id_type=MESH,
        )

    tall_own = pltpu.make_async_copy(
        d_loc.at[pl.ds(fs * held, held)],
        d_out.at[gr, :, pl.ds(pl.multiple_of(fs * rows, rows), rows), :],
        own.at[2],
    )
    pairs = ((g_loc, g_out, 0), (u_loc, u_out, 1))
    order = [d for d in range(1, n_fs)] + [0]
    for loc, out, m in pairs:
        for d in order:
            if d:
                wide(loc, out, m, d).start()
            else:
                @pl.when(to_tp == tp)
                def _():
                    wide_own(loc, out, m).start()

                @pl.when(to_tp != tp)
                def _():
                    wide(loc, out, m, 0).start()
    for d in range(1, n_fs):
        tall(d).start()
    tall_own.start()

    def forward(block, s_sem, r_sem, p):
        return pltpu.make_async_remote_copy(
            src_ref=block, dst_ref=block, send_sem=s_sem, recv_sem=r_sem,
            device_id=((gr + p) % n_gr, fs, tp), device_id_type=MESH,
        )

    def landed(block, r_sem):
        pltpu.make_async_remote_copy(
            src_ref=block, dst_ref=block, send_sem=r_sem, recv_sem=r_sem,
            device_id=((gr + 1) % n_gr, fs, tp), device_id_type=MESH,
        ).wait_recv()

    def wide_block(out, g, j, t):
        return out.at[g, :, pl.ds(j * rows, rows), pl.ds(t * cols, cols)]

    for loc, out, m in pairs:
        for j in range(per):
            for t in range(n_tp):
                here = (tp * per + j == fs) & (tp == t)

                @pl.when(here)
                def _():
                    wide_own(loc, out, m).wait()

                @pl.when(jnp.logical_not(here))
                def _():
                    landed(wide_block(out, gr, j, t), recv.at[m, j, t])
                for p in range(1, n_gr):
                    forward(wide_block(out, gr, j, t), f_send.at[m, j, t, p - 1],
                            f_recv.at[m, j, t, p - 1], p).start()

    def tall_block(g, s):
        return d_out.at[g, :, pl.ds(s * rows, rows), :]

    for s in range(n_fs):
        @pl.when(s == fs)
        def _():
            tall_own.wait()

        @pl.when(s != fs)
        def _():
            landed(tall_block(gr, s), d_recv.at[s])
        for p in range(1, n_gr):
            forward(tall_block(gr, s), fd_send.at[s, p - 1], fd_recv.at[s, p - 1], p).start()

    for loc, out, m in pairs:
        for d in order:
            if d:
                wide(loc, out, m, d).wait_send()
            else:
                @pl.when(to_tp != tp)
                def _():
                    wide(loc, out, m, 0).wait_send()
        for j in range(per):
            for t in range(n_tp):
                for p in range(1, n_gr):
                    forward(wide_block(out, gr, j, t), f_send.at[m, j, t, p - 1],
                            f_recv.at[m, j, t, p - 1], p).wait_send()
                    landed(wide_block(out, (gr + n_gr - p) % n_gr, j, t), f_recv.at[m, j, t, p - 1])
    for d in range(1, n_fs):
        tall(d).wait_send()
    for s in range(n_fs):
        for p in range(1, n_gr):
            forward(tall_block(gr, s), fd_send.at[s, p - 1], fd_recv.at[s, p - 1], p).wait_send()
            landed(tall_block((gr + n_gr - p) % n_gr, s), fd_recv.at[s, p - 1])


def exchange(dims, g_loc, u_loc, d_loc):
    n_gr, n_fs, n_tp = dims
    count, rows, cols = g_loc.shape
    held = count // n_fs
    units = n_fs * rows
    bf = jnp.bfloat16
    per = units // n_tp // rows
    dma = pltpu.SemaphoreType.DMA
    wide = jax.ShapeDtypeStruct((n_gr, held, units // n_tp, n_tp * cols), bf)
    tall = jax.ShapeDtypeStruct((n_gr, held, units, cols), bf)
    sent = 3 * count * rows * cols * 2

    def body(*refs):
        exchange_kernel(dims, *refs)

    return pl.pallas_call(
        body,
        out_shape=(wide, wide, tall),
        in_specs=[pl.BlockSpec(memory_space=pl.ANY)] * 3,
        out_specs=[pl.BlockSpec(memory_space=pl.ANY)] * 3,
        scratch_shapes=[
            dma((2, n_fs)), dma((2, per, n_tp)), dma((n_fs,)), dma((n_fs,)), dma((3,)),
            dma((2, per, n_tp, n_gr - 1)), dma((2, per, n_tp, n_gr - 1)),
            dma((n_fs, n_gr - 1)), dma((n_fs, n_gr - 1)),
        ],
        compiler_params=pltpu.CompilerParams(collective_id=1, has_side_effects=True),
        cost_estimate=pl.CostEstimate(flops=0, bytes_accessed=100 * sent, transcendentals=0),
    )(g_loc, u_loc, d_loc)


def on_device(tokens, routes, route_weight, norm_gain, gate_experts, up_experts, down_experts,
              gate_shared, up_shared, down_shared):
    bf = jnp.bfloat16
    f32 = jnp.float32
    dims = (lax.axis_size("gr"), lax.axis_size("fs"), lax.axis_size("tp"))
    n_gr, n_fs, n_tp = dims
    fs_index = lax.axis_index("fs")
    tp_index = lax.axis_index("tp")
    cols = gate_experts.shape[3]
    per_group = gate_experts.shape[1]
    count = per_group * n_gr
    held = per_group // n_fs
    tok_count, top = routes.shape
    width = tokens.shape[1]

    values = tokens.astype(f32)
    normed = (values * lax.rsqrt(jnp.mean(values * values, axis=-1, keepdims=True) + EPS)).astype(bf)
    named = routes[:, :, None] == jnp.arange(count, dtype=jnp.int32)[None, None, :]
    weight = jnp.sum(jnp.where(named, route_weight[:, :, None], 0.0), axis=1)
    high = lax.reduce_precision(weight, 8, 7)
    extra = -(-2 * count // 128) * 128
    tail = jnp.concatenate(
        [high.astype(bf), (weight - high).astype(bf), jnp.zeros((tok_count, extra - 2 * count), bf)],
        axis=1,
    )
    rows_all = lax.all_gather(jnp.concatenate([normed, tail], axis=1), "fs", axis=0, tiled=True)

    gain_shared = lax.dynamic_slice_in_dim(
        norm_gain, fs_index * gate_shared.shape[0], gate_shared.shape[0], 0
    )
    gate_sw = lax.all_gather((gate_shared * gain_shared[:, None]).astype(bf), "fs", axis=0, tiled=True)
    up_sw = lax.all_gather((up_shared * gain_shared[:, None]).astype(bf), "fs", axis=0, tiled=True)
    down_sw = lax.all_gather(down_shared.astype(bf), "fs", axis=0, tiled=True)

    gain_cols = lax.dynamic_slice_in_dim(norm_gain, tp_index * cols, cols, 0)
    gate_w, up_w, down_w = exchange(
        dims,
        (gate_experts[0] * gain_cols[None, None, :]).astype(bf),
        (up_experts[0] * gain_cols[None, None, :]).astype(bf),
        down_experts[0].astype(bf),
    )

    x = rows_all[:, :width]
    w_all = (
        rows_all[:, width:width + count].astype(f32)
        + rows_all[:, width + count:width + 2 * count].astype(f32)
    )
    units = gate_w.shape[2]
    parts = []
    for g in range(n_gr):
        w_here = lax.dynamic_slice_in_dim(w_all, g * per_group + fs_index * held, held, 1)
        for k in range(held):
            gate = lax.dot_general(x, gate_w[g, k], (((1,), (1,)), ((), ())), preferred_element_type=f32)
            upper = lax.dot_general(x, up_w[g, k], (((1,), (1,)), ((), ())), preferred_element_type=f32)
            parts.append((jax.nn.silu(gate) * upper * w_here[:, k:k + 1]).astype(bf))
    hidden = jnp.stack(parts)
    hidden = lax.all_gather(hidden, "tp", axis=0, tiled=False)
    partial = jnp.zeros((), f32)
    down_flat = down_w.reshape(n_gr * held, n_tp, units, cols)
    for i in range(n_gr * held):
        for t in range(n_tp):
            partial = partial + jnp.dot(hidden[t, i], down_flat[i, t], preferred_element_type=f32)
    routed = lax.psum_scatter(partial.astype(bf), "fs", scatter_dimension=0, tiled=True)

    shared_hidden = (
        jax.nn.silu(jnp.dot(normed, gate_sw, preferred_element_type=f32))
        * jnp.dot(normed, up_sw, preferred_element_type=f32)
    ).astype(bf)
    shared_full = lax.all_gather(shared_hidden, "tp", axis=1, tiled=True)
    shared = jnp.dot(shared_full, down_sw, preferred_element_type=f32)
    mixed = (routed.astype(f32) + shared).astype(bf)
    return (mixed, gate_w, up_w, down_w, gate_sw, up_sw, down_sw)


def solution(mesh):
    return jax.shard_map(
        on_device,
        mesh=mesh,
        in_specs=(
            P(("gr", "fs"), None),
            P(("gr", "fs"), None),
            P(("gr", "fs"), None),
            P(),
            P("gr", None, "fs", "tp"),
            P("gr", None, "fs", "tp"),
            P("gr", None, "fs", "tp"),
            P("fs", "tp"),
            P("fs", "tp"),
            P("fs", "tp"),
        ),
        out_specs=(
            P(("gr", "fs"), "tp"),
            P(None, "fs", "tp", None),
            P(None, "fs", "tp", None),
            P(None, "fs", None, "tp"),
            P(None, "tp"),
            P(None, "tp"),
            P(None, "tp"),
        ),
        check_vma=False,
    )
```

```python
import functools

import jax
import jax.numpy as jnp
from jax import lax
from jax.experimental import pallas as pl
from jax.experimental.pallas import tpu as pltpu
from jax.sharding import PartitionSpec as P

EPS = 1e-06
MESH = pl.DeviceIdType.MESH


def greet_group(dims, gr, fs, tp, barrier):
    n_gr, n_fs, n_tp = dims

    def greet(i, carry):
        f, t = i // n_tp, i % n_tp

        @pl.when((f != fs) | (t != tp))
        def _():
            pl.semaphore_signal(barrier, inc=1, device_id=(gr, f, t), device_id_type=MESH)
        return carry

    lax.fori_loop(0, n_fs * n_tp, greet, 0)
    for p in range(1, n_gr):
        pl.semaphore_signal(
            barrier, inc=1, device_id=((gr + p) % n_gr, fs, tp), device_id_type=MESH
        )
    pl.semaphore_wait(barrier, n_fs * n_tp - 1 + n_gr - 1)


def forward(n_gr, block, s_sem, r_sem, p):
    gr, fs, tp = lax.axis_index("gr"), lax.axis_index("fs"), lax.axis_index("tp")
    return pltpu.make_async_remote_copy(
        src_ref=block, dst_ref=block, send_sem=s_sem, recv_sem=r_sem,
        device_id=((gr + p) % n_gr, fs, tp), device_id_type=MESH,
    )


def wide_kernel(dims, g_loc, u_loc, g_out, u_out, send, recv, own, f_send, f_recv):
    n_gr, n_fs, n_tp = dims
    gr, fs, tp = lax.axis_index("gr"), lax.axis_index("fs"), lax.axis_index("tp")
    held = g_loc.shape[0] // n_fs
    rows, cols = g_loc.shape[1], g_loc.shape[2]
    per = g_out.shape[2] // rows
    greet_group(dims, gr, fs, tp, pltpu.get_barrier_semaphore())
    to_tp = fs // per

    def place(out):
        return out.at[gr, :, pl.ds(pl.multiple_of((fs % per) * rows, rows), rows),
                      pl.ds(pl.multiple_of(tp * cols, cols), cols)]

    def wide(loc, out, m, d):
        k = (fs + d) % n_fs
        return pltpu.make_async_remote_copy(
            src_ref=loc.at[pl.ds(k * held, held)], dst_ref=place(out),
            send_sem=send.at[m, d], recv_sem=recv.at[m, fs % per, tp],
            device_id=(gr, k, to_tp), device_id_type=MESH,
        )

    def wide_own(loc, out, m):
        return pltpu.make_async_copy(loc.at[pl.ds(fs * held, held)], place(out), own.at[m])

    def block(out, g, j, t):
        return out.at[g, :, pl.ds(j * rows, rows), pl.ds(t * cols, cols)]

    pairs = ((g_loc, g_out, 0), (u_loc, u_out, 1))
    for loc, out, m in pairs:
        for d in range(1, n_fs):
            wide(loc, out, m, d).start()

        @pl.when(to_tp == tp)
        def _():
            wide_own(loc, out, m).start()

        @pl.when(to_tp != tp)
        def _():
            wide(loc, out, m, 0).start()
    for loc, out, m in pairs:
        for j in range(per):
            for t in range(n_tp):
                here = (tp * per + j == fs) & (tp == t)
                part = block(out, gr, j, t)

                @pl.when(here)
                def _():
                    wide_own(loc, out, m).wait()

                @pl.when(jnp.logical_not(here))
                def _():
                    forward(n_gr, part, recv.at[m, j, t], recv.at[m, j, t], 1).wait_recv()
                for p in range(1, n_gr):
                    forward(n_gr, part, f_send.at[m, j, t, p - 1], f_recv.at[m, j, t, p - 1], p).start()
    for loc, out, m in pairs:
        for d in range(1, n_fs):
            wide(loc, out, m, d).wait_send()

        @pl.when(to_tp != tp)
        def _():
            wide(loc, out, m, 0).wait_send()
        for j in range(per):
            for t in range(n_tp):
                for p in range(1, n_gr):
                    sems = f_send.at[m, j, t, p - 1], f_recv.at[m, j, t, p - 1]
                    forward(n_gr, block(out, gr, j, t), *sems, p).wait_send()
                    forward(n_gr, block(out, (gr + n_gr - p) % n_gr, j, t), *sems, p).wait_recv()


def tall_kernel(dims, d_loc, d_out, send, recv, own, f_send, f_recv):
    n_gr, n_fs, n_tp = dims
    gr, fs, tp = lax.axis_index("gr"), lax.axis_index("fs"), lax.axis_index("tp")
    held = d_loc.shape[0] // n_fs
    rows = d_loc.shape[1]
    greet_group(dims, gr, fs, tp, pltpu.get_barrier_semaphore())

    def block(g, s):
        start = s * rows if isinstance(s, int) else pl.multiple_of(s * rows, rows)
        return d_out.at[g, :, pl.ds(start, rows), :]

    def tall(d):
        k = (fs + d) % n_fs
        return pltpu.make_async_remote_copy(
            src_ref=d_loc.at[pl.ds(k * held, held)], dst_ref=block(gr, fs),
            send_sem=send.at[d], recv_sem=recv.at[fs],
            device_id=(gr, k, tp), device_id_type=MESH,
        )

    mine = pltpu.make_async_copy(d_loc.at[pl.ds(fs * held, held)], block(gr, fs), own)
    for d in range(1, n_fs):
        tall(d).start()
    mine.start()
    for s in range(n_fs):
        @pl.when(s == fs)
        def _():
            mine.wait()

        @pl.when(s != fs)
        def _():
            forward(n_gr, block(gr, s), recv.at[s], recv.at[s], 1).wait_recv()
        for p in range(1, n_gr):
            forward(n_gr, block(gr, s), f_send.at[s, p - 1], f_recv.at[s, p - 1], p).start()
    for d in range(1, n_fs):
        tall(d).wait_send()
    for s in range(n_fs):
        for p in range(1, n_gr):
            sems = f_send.at[s, p - 1], f_recv.at[s, p - 1]
            forward(n_gr, block(gr, s), *sems, p).wait_send()
            forward(n_gr, block((gr + n_gr - p) % n_gr, s), *sems, p).wait_recv()


def gather_kernel(dims, inner, number, *refs):
    n_gr, n_fs, n_tp = dims
    gr, fs, tp = lax.axis_index("gr"), lax.axis_index("fs"), lax.axis_index("tp")
    ins, outs = refs[:number], refs[number:2 * number]
    z_send, z_recv, y_send, y_recv, own = refs[2 * number:]
    nz = n_fs // inner
    z, y = fs // inner, fs % inner
    barrier = pltpu.get_barrier_semaphore()

    def when_next(way, act):
        pl.when(z < nz - 1 if way == 0 else z > 0)(act)

    def beside(way):
        return (gr, (z + 1 if way == 0 else z - 1) * inner + y, tp)

    for q in range(1, inner):
        pl.semaphore_signal(barrier, inc=1, device_id=(gr, z * inner + (y + q) % inner, tp), device_id_type=MESH)
    for way in (0, 1):
        when_next(way, lambda way=way: pl.semaphore_signal(
            barrier, inc=1, device_id=beside(way), device_id_type=MESH))
    peers = inner - 1 + (z > 0).astype(jnp.int32) + (z < nz - 1).astype(jnp.int32)
    pl.semaphore_wait(barrier, peers)

    def block(m, zz, yy):
        rows = ins[m].shape[0]
        return outs[m].at[pl.ds(pl.multiple_of((zz * inner + yy) * rows, rows), rows), :]

    def at(way, d):
        return z - d if way == 0 else z + d

    def z_copy(m, way, d):
        return pltpu.make_async_remote_copy(
            src_ref=ins[m] if d == 0 else block(m, at(way, d), y), dst_ref=block(m, at(way, d), y),
            send_sem=z_send.at[m, way, d], recv_sem=z_recv.at[m, way, d],
            device_id=beside(way), device_id_type=MESH,
        )

    def z_landed(m, way, d):
        part = block(m, at(way, d), y)
        pltpu.make_async_remote_copy(
            src_ref=part, dst_ref=part, send_sem=z_send.at[m, way, d - 1],
            recv_sem=z_recv.at[m, way, d - 1], device_id=beside(way), device_id_type=MESH,
        ).wait_recv()

    def y_copy(m, q, way, d, source):
        part = block(m, at(way, d), source)
        i = d + way * (nz - 1) if d else 0
        return pltpu.make_async_remote_copy(
            src_ref=ins[m] if d == 0 else part, dst_ref=part,
            send_sem=y_send.at[m, q - 1, i], recv_sem=y_recv.at[m, q - 1, i],
            device_id=(gr, z * inner + (y + q) % inner, tp), device_id_type=MESH,
        )

    def own_copy(m):
        return pltpu.make_async_copy(ins[m], block(m, z, y), own.at[m])

    def steps(d, way, act):
        if d == 0:
            act()
        else:
            pl.when(z - d >= 0 if way == 0 else z + d < nz)(act)

    places = [(0, 0)] + [(d, way) for d in range(1, nz) for way in (0, 1)]
    for m in range(number):
        for way in (0, 1):
            when_next(way, lambda m=m, way=way: z_copy(m, way, 0).start())
        for q in range(1, inner):
            y_copy(m, q, 0, 0, y).start()
    for m in range(number):
        own_copy(m).start()
    for d, way in places[1:]:
        def pass_on(d=d, way=way):
            for m in range(number):
                z_landed(m, way, d)
                if d < nz - 1:
                    when_next(way, lambda: z_copy(m, way, d).start())
                for q in range(1, inner):
                    y_copy(m, q, way, d, y).start()
        steps(d, way, pass_on)
    for m in range(number):
        for way in (0, 1):
            when_next(way, lambda m=m, way=way: z_copy(m, way, 0).wait_send())
    for d, way in places:
        def finish(d=d, way=way):
            for m in range(number):
                if 0 < d < nz - 1:
                    when_next(way, lambda: z_copy(m, way, d).wait_send())
                for q in range(1, inner):
                    y_copy(m, q, way, d, y).wait_send()
                    y_copy(m, q, way, d, (y + inner - q) % inner).wait_recv()
        steps(d, way, finish)
    for m in range(number):
        own_copy(m).wait()


def call(body, outs, sems, ident, work, *args):
    return pl.pallas_call(
        body,
        out_shape=outs,
        in_specs=[pl.BlockSpec(memory_space=pl.ANY)] * len(args),
        out_specs=tuple(pl.BlockSpec(memory_space=pl.ANY) for _ in outs),
        scratch_shapes=[pltpu.SemaphoreType.DMA(shape) for shape in sems],
        compiler_params=pltpu.CompilerParams(collective_id=ident, has_side_effects=True),
        cost_estimate=pl.CostEstimate(flops=0, bytes_accessed=work, transcendentals=0),
    )(*args)


def exchange_wide(dims, g_loc, u_loc):
    n_gr, n_fs, n_tp = dims
    count, rows, cols = g_loc.shape
    per = n_fs // n_tp
    out = jax.ShapeDtypeStruct((n_gr, count // n_fs, per * rows, n_tp * cols), g_loc.dtype)
    halves = (2, per, n_tp, n_gr - 1)
    return call(
        functools.partial(wide_kernel, dims), (out, out),
        [(2, n_fs), (2, per, n_tp), (2,), halves, halves], 1, 200 << 20, g_loc, u_loc,
    )


def exchange_tall(dims, d_loc):
    n_gr, n_fs, n_tp = dims
    count, rows, cols = d_loc.shape
    out = jax.ShapeDtypeStruct((n_gr, count // n_fs, n_fs * rows, cols), d_loc.dtype)
    return call(
        functools.partial(tall_kernel, dims), (out,),
        [(n_fs,), (n_fs,), (), (n_fs, n_gr - 1), (n_fs, n_gr - 1)], 2, 100 << 20, d_loc,
    )[0]


def gather_fs(dims, ident, work, *arrays):
    n_fs = dims[1]
    inner = 2 if n_fs % 2 == 0 else 1
    nz = n_fs // inner
    number = len(arrays)
    outs = tuple(jax.ShapeDtypeStruct((n_fs * a.shape[0], a.shape[1]), a.dtype) for a in arrays)
    chain = (number, 2, max(1, nz - 1))
    across = (number, max(1, inner - 1), 2 * nz - 1)
    return call(
        functools.partial(gather_kernel, dims, inner, number), outs,
        [chain, chain, across, across, (number,)], ident, work, *arrays,
    )


def on_device(tokens, routes, route_weight, norm_gain, gate_experts, up_experts, down_experts,
              gate_shared, up_shared, down_shared):
    bf = jnp.bfloat16
    f32 = jnp.float32
    dims = (lax.axis_size("gr"), lax.axis_size("fs"), lax.axis_size("tp"))
    n_gr, n_fs, n_tp = dims
    fs_index = lax.axis_index("fs")
    tp_index = lax.axis_index("tp")
    cols = gate_experts.shape[3]
    per_group = gate_experts.shape[1]
    count = per_group * n_gr
    held = per_group // n_fs
    tok_count, top = routes.shape
    width = tokens.shape[1]

    values = tokens.astype(f32)
    normed = (values * lax.rsqrt(jnp.mean(values * values, axis=-1, keepdims=True) + EPS)).astype(bf)
    named = routes[:, :, None] == jnp.arange(count, dtype=jnp.int32)[None, None, :]
    weight = jnp.sum(jnp.where(named, route_weight[:, :, None], 0.0), axis=1)
    high = lax.reduce_precision(weight, 8, 7)
    extra = -(-2 * count // 128) * 128
    tail = jnp.concatenate(
        [high.astype(bf), (weight - high).astype(bf), jnp.zeros((tok_count, extra - 2 * count), bf)],
        axis=1,
    )
    rows_all = lax.all_gather(jnp.concatenate([normed, tail], axis=1), "fs", axis=0, tiled=True)

    gain_shared = lax.dynamic_slice_in_dim(
        norm_gain, fs_index * gate_shared.shape[0], gate_shared.shape[0], 0
    )
    shared_here = (
        (gate_shared * gain_shared[:, None]).astype(bf),
        (up_shared * gain_shared[:, None]).astype(bf),
        down_shared.astype(bf),
    )

    gain_cols = lax.dynamic_slice_in_dim(norm_gain, tp_index * cols, cols, 0)
    gate_w, up_w = exchange_wide(
        dims,
        (gate_experts[0] * gain_cols[None, None, :]).astype(bf),
        (up_experts[0] * gain_cols[None, None, :]).astype(bf),
    )

    x = rows_all[:, :width]
    w_all = (
        rows_all[:, width:width + count].astype(f32)
        + rows_all[:, width + count:width + 2 * count].astype(f32)
    )
    units = gate_w.shape[2]
    parts = []
    for g in range(n_gr):
        w_here = lax.dynamic_slice_in_dim(w_all, g * per_group + fs_index * held, held, 1)
        for k in range(held):
            gate = lax.dot_general(x, gate_w[g, k], (((1,), (1,)), ((), ())), preferred_element_type=f32)
            upper = lax.dot_general(x, up_w[g, k], (((1,), (1,)), ((), ())), preferred_element_type=f32)
            parts.append((jax.nn.silu(gate) * upper * w_here[:, k:k + 1]).astype(bf))
    hidden = jnp.stack(parts)
    hidden, down_local = lax.optimization_barrier((hidden, down_experts[0].astype(bf)))
    down_w = exchange_tall(dims, down_local)
    hidden = lax.all_gather(hidden, "tp", axis=0, tiled=False)
    partial = jnp.zeros((), f32)
    down_flat = down_w.reshape(n_gr * held, n_tp, units, cols)
    for i in range(n_gr * held):
        for t in range(n_tp):
            partial = partial + jnp.dot(hidden[t, i], down_flat[i, t], preferred_element_type=f32)
    partial, shared_here = lax.optimization_barrier((partial.astype(bf), shared_here))
    gate_sw, up_sw, down_sw = gather_fs(dims, 3, 60 << 20, *shared_here)
    routed = lax.psum_scatter(partial, "fs", scatter_dimension=0, tiled=True)

    shared_hidden = (
        jax.nn.silu(jnp.dot(normed, gate_sw, preferred_element_type=f32))
        * jnp.dot(normed, up_sw, preferred_element_type=f32)
    ).astype(bf)
    shared_full = lax.all_gather(shared_hidden, "tp", axis=1, tiled=True)
    shared = jnp.dot(shared_full, down_sw, preferred_element_type=f32)
    mixed = (routed.astype(f32) + shared).astype(bf)
    return (mixed, gate_w, up_w, down_w, gate_sw, up_sw, down_sw)


def solution(mesh):
    return jax.shard_map(
        on_device,
        mesh=mesh,
        in_specs=(
            P(("gr", "fs"), None),
            P(("gr", "fs"), None),
            P(("gr", "fs"), None),
            P(),
            P("gr", None, "fs", "tp"),
            P("gr", None, "fs", "tp"),
            P("gr", None, "fs", "tp"),
            P("fs", "tp"),
            P("fs", "tp"),
            P("fs", "tp"),
        ),
        out_specs=(
            P(("gr", "fs"), "tp"),
            P(None, "fs", "tp", None),
            P(None, "fs", "tp", None),
            P(None, "fs", None, "tp"),
            P(None, "tp"),
            P(None, "tp"),
            P(None, "tp"),
        ),
        check_vma=False,
    )
```

```python
import functools

import jax
import jax.numpy as jnp
from jax import lax
from jax.experimental import pallas as pl
from jax.experimental.pallas import tpu as pltpu
from jax.sharding import PartitionSpec as P

EPS = 1e-06
MESH = pl.DeviceIdType.MESH


def greet_group(dims, gr, fs, tp, barrier):
    n_gr, n_fs, n_tp = dims

    def greet(i, carry):
        f, t = i // n_tp, i % n_tp

        @pl.when((f != fs) | (t != tp))
        def _():
            pl.semaphore_signal(barrier, inc=1, device_id=(gr, f, t), device_id_type=MESH)
        return carry

    lax.fori_loop(0, n_fs * n_tp, greet, 0)
    for p in range(1, n_gr):
        pl.semaphore_signal(
            barrier, inc=1, device_id=((gr + p) % n_gr, fs, tp), device_id_type=MESH
        )
    pl.semaphore_wait(barrier, n_fs * n_tp - 1 + n_gr - 1)


def forward(n_gr, block, s_sem, r_sem, p):
    gr, fs, tp = lax.axis_index("gr"), lax.axis_index("fs"), lax.axis_index("tp")
    return pltpu.make_async_remote_copy(
        src_ref=block, dst_ref=block, send_sem=s_sem, recv_sem=r_sem,
        device_id=((gr + p) % n_gr, fs, tp), device_id_type=MESH,
    )


def wide_steps(dims, g_loc, u_loc, g_out, u_out, send, recv, own, f_send, f_recv):
    n_gr, n_fs, n_tp = dims
    gr, fs, tp = lax.axis_index("gr"), lax.axis_index("fs"), lax.axis_index("tp")
    held = g_loc.shape[0] // n_fs
    rows, cols = g_loc.shape[1], g_loc.shape[2]
    per = g_out.shape[2] // rows
    to_tp = fs // per

    def place(out):
        return out.at[gr, :, pl.ds(pl.multiple_of((fs % per) * rows, rows), rows),
                      pl.ds(pl.multiple_of(tp * cols, cols), cols)]

    def wide(loc, out, m, d):
        k = (fs + d) % n_fs
        return pltpu.make_async_remote_copy(
            src_ref=loc.at[pl.ds(k * held, held)], dst_ref=place(out),
            send_sem=send.at[m, d], recv_sem=recv.at[m, fs % per, tp],
            device_id=(gr, k, to_tp), device_id_type=MESH,
        )

    def wide_own(loc, out, m):
        return pltpu.make_async_copy(loc.at[pl.ds(fs * held, held)], place(out), own.at[m])

    def block(out, g, j, t):
        return out.at[g, :, pl.ds(j * rows, rows), pl.ds(t * cols, cols)]

    pairs = ((g_loc, g_out, 0), (u_loc, u_out, 1))
    for loc, out, m in pairs:
        for d in range(1, n_fs):
            wide(loc, out, m, d).start()

        @pl.when(to_tp == tp)
        def _():
            wide_own(loc, out, m).start()

        @pl.when(to_tp != tp)
        def _():
            wide(loc, out, m, 0).start()
        yield
    for loc, out, m in pairs:
        for j in range(per):
            for t in range(n_tp):
                here = (tp * per + j == fs) & (tp == t)
                part = block(out, gr, j, t)

                @pl.when(here)
                def _():
                    wide_own(loc, out, m).wait()

                @pl.when(jnp.logical_not(here))
                def _():
                    forward(n_gr, part, recv.at[m, j, t], recv.at[m, j, t], 1).wait_recv()
                for p in range(1, n_gr):
                    forward(n_gr, part, f_send.at[m, j, t, p - 1], f_recv.at[m, j, t, p - 1], p).start()
        yield
    for loc, out, m in pairs:
        for d in range(1, n_fs):
            wide(loc, out, m, d).wait_send()

        @pl.when(to_tp != tp)
        def _():
            wide(loc, out, m, 0).wait_send()
        for j in range(per):
            for t in range(n_tp):
                for p in range(1, n_gr):
                    sems = f_send.at[m, j, t, p - 1], f_recv.at[m, j, t, p - 1]
                    forward(n_gr, block(out, gr, j, t), *sems, p).wait_send()
                    forward(n_gr, block(out, (gr + n_gr - p) % n_gr, j, t), *sems, p).wait_recv()


def tall_steps(dims, d_loc, d_out, send, recv, own, f_send, f_recv):
    n_gr, n_fs, n_tp = dims
    gr, fs, tp = lax.axis_index("gr"), lax.axis_index("fs"), lax.axis_index("tp")
    held = d_loc.shape[0] // n_fs
    rows = d_loc.shape[1]

    def block(g, s):
        start = s * rows if isinstance(s, int) else pl.multiple_of(s * rows, rows)
        return d_out.at[g, :, pl.ds(start, rows), :]

    def tall(d):
        k = (fs + d) % n_fs
        return pltpu.make_async_remote_copy(
            src_ref=d_loc.at[pl.ds(k * held, held)], dst_ref=block(gr, fs),
            send_sem=send.at[d], recv_sem=recv.at[fs],
            device_id=(gr, k, tp), device_id_type=MESH,
        )

    mine = pltpu.make_async_copy(d_loc.at[pl.ds(fs * held, held)], block(gr, fs), own)
    for d in range(1, n_fs):
        tall(d).start()
    mine.start()
    yield
    for s in range(n_fs):
        @pl.when(s == fs)
        def _():
            mine.wait()

        @pl.when(s != fs)
        def _():
            forward(n_gr, block(gr, s), recv.at[s], recv.at[s], 1).wait_recv()
        for p in range(1, n_gr):
            forward(n_gr, block(gr, s), f_send.at[s, p - 1], f_recv.at[s, p - 1], p).start()
    yield
    for d in range(1, n_fs):
        tall(d).wait_send()
    for s in range(n_fs):
        for p in range(1, n_gr):
            sems = f_send.at[s, p - 1], f_recv.at[s, p - 1]
            forward(n_gr, block(gr, s), *sems, p).wait_send()
            forward(n_gr, block((gr + n_gr - p) % n_gr, s), *sems, p).wait_recv()


def gather_steps(dims, inner, number, *refs):
    n_gr, n_fs, n_tp = dims
    gr, fs, tp = lax.axis_index("gr"), lax.axis_index("fs"), lax.axis_index("tp")
    ins, outs = refs[:number], refs[number:2 * number]
    z_send, z_recv, y_send, y_recv, own = refs[2 * number:]
    nz = n_fs // inner
    z, y = fs // inner, fs % inner

    def when_next(way, act):
        pl.when(z < nz - 1 if way == 0 else z > 0)(act)

    def beside(way):
        return (gr, (z + 1 if way == 0 else z - 1) * inner + y, tp)

    def block(m, zz, yy):
        rows = ins[m].shape[0]
        return outs[m].at[pl.ds(pl.multiple_of((zz * inner + yy) * rows, rows), rows), :]

    def at(way, d):
        return z - d if way == 0 else z + d

    def z_copy(m, way, d):
        return pltpu.make_async_remote_copy(
            src_ref=ins[m] if d == 0 else block(m, at(way, d), y), dst_ref=block(m, at(way, d), y),
            send_sem=z_send.at[m, way, d], recv_sem=z_recv.at[m, way, d],
            device_id=beside(way), device_id_type=MESH,
        )

    def z_landed(m, way, d):
        part = block(m, at(way, d), y)
        pltpu.make_async_remote_copy(
            src_ref=part, dst_ref=part, send_sem=z_send.at[m, way, d - 1],
            recv_sem=z_recv.at[m, way, d - 1], device_id=beside(way), device_id_type=MESH,
        ).wait_recv()

    def y_copy(m, q, way, d, source):
        part = block(m, at(way, d), source)
        i = d + way * (nz - 1) if d else 0
        return pltpu.make_async_remote_copy(
            src_ref=ins[m] if d == 0 else part, dst_ref=part,
            send_sem=y_send.at[m, q - 1, i], recv_sem=y_recv.at[m, q - 1, i],
            device_id=(gr, z * inner + (y + q) % inner, tp), device_id_type=MESH,
        )

    def own_copy(m):
        return pltpu.make_async_copy(ins[m], block(m, z, y), own.at[m])

    def steps(d, way, act):
        if d == 0:
            act()
        else:
            pl.when(z - d >= 0 if way == 0 else z + d < nz)(act)

    places = [(0, 0)] + [(d, way) for d in range(1, nz) for way in (0, 1)]
    for m in range(number):
        for way in (0, 1):
            when_next(way, lambda m=m, way=way: z_copy(m, way, 0).start())
        for q in range(1, inner):
            y_copy(m, q, 0, 0, y).start()
    for m in range(number):
        own_copy(m).start()
    yield
    for d, way in places[1:]:
        def pass_on(d=d, way=way):
            for m in range(number):
                z_landed(m, way, d)
                if d < nz - 1:
                    when_next(way, lambda: z_copy(m, way, d).start())
                for q in range(1, inner):
                    y_copy(m, q, way, d, y).start()
        steps(d, way, pass_on)
        if way:
            yield
    for m in range(number):
        for way in (0, 1):
            when_next(way, lambda m=m, way=way: z_copy(m, way, 0).wait_send())
    for d, way in places:
        def finish(d=d, way=way):
            for m in range(number):
                if 0 < d < nz - 1:
                    when_next(way, lambda: z_copy(m, way, d).wait_send())
                for q in range(1, inner):
                    y_copy(m, q, way, d, y).wait_send()
                    y_copy(m, q, way, d, (y + inner - q) % inner).wait_recv()
        steps(d, way, finish)
    for m in range(number):
        own_copy(m).wait()


def run_steps(first, second):
    live = [first, second]
    while live:
        for steps in list(live):
            if next(steps, live) is live:
                live.remove(steps)


def fused_kernel(dims, inner, number, main_steps, main_ins, main_outs, main_sems, *refs):
    gr, fs, tp = lax.axis_index("gr"), lax.axis_index("fs"), lax.axis_index("tp")
    greet_group(dims, gr, fs, tp, pltpu.get_barrier_semaphore())
    edges = [0]
    for n in (number, main_ins, number, main_outs, 5, main_sems):
        edges.append(edges[-1] + n)
    a, b, c, d, e, f = [refs[edges[i]:edges[i + 1]] for i in range(6)]
    run_steps(gather_steps(dims, inner, number, *a, *c, *e), main_steps(dims, *b, *d, *f))


def exchange(dims, ident, work, main_steps, arrays, main_args, main_outs, main_sems):
    n_fs = dims[1]
    inner = 2 if n_fs % 2 == 0 else 1
    nz = n_fs // inner
    number = len(arrays)
    outs = tuple(jax.ShapeDtypeStruct((n_fs * a.shape[0], a.shape[1]), a.dtype) for a in arrays)
    chain = (number, 2, max(1, nz - 1))
    across = (number, max(1, inner - 1), 2 * nz - 1)
    sems = [chain, chain, across, across, (number,), *main_sems]
    args = (*arrays, *main_args)
    outs = outs + tuple(main_outs)
    return pl.pallas_call(
        functools.partial(
            fused_kernel, dims, inner, number, main_steps,
            len(main_args), len(main_outs), len(main_sems),
        ),
        out_shape=outs,
        in_specs=[pl.BlockSpec(memory_space=pl.ANY)] * len(args),
        out_specs=tuple(pl.BlockSpec(memory_space=pl.ANY) for _ in outs),
        scratch_shapes=[pltpu.SemaphoreType.DMA(shape) for shape in sems],
        compiler_params=pltpu.CompilerParams(collective_id=ident, has_side_effects=True),
        cost_estimate=pl.CostEstimate(flops=0, bytes_accessed=work, transcendentals=0),
    )(*args)


def exchange_wide(dims, rows_here, g_loc, u_loc):
    n_gr, n_fs, n_tp = dims
    count, rows, cols = g_loc.shape
    per = n_fs // n_tp
    out = jax.ShapeDtypeStruct((n_gr, count // n_fs, per * rows, n_tp * cols), g_loc.dtype)
    halves = (2, per, n_tp, n_gr - 1)
    return exchange(
        dims, 1, 200 << 20, wide_steps, (rows_here,), (g_loc, u_loc), (out, out),
        [(2, n_fs), (2, per, n_tp), (2,), halves, halves],
    )


def exchange_tall(dims, shared_here, d_loc):
    n_gr, n_fs, n_tp = dims
    count, rows, cols = d_loc.shape
    out = jax.ShapeDtypeStruct((n_gr, count // n_fs, n_fs * rows, cols), d_loc.dtype)
    return exchange(
        dims, 2, 100 << 20, tall_steps, shared_here, (d_loc,), (out,),
        [(n_fs,), (n_fs,), (), (n_fs, n_gr - 1), (n_fs, n_gr - 1)],
    )


def on_device(tokens, routes, route_weight, norm_gain, gate_experts, up_experts, down_experts,
              gate_shared, up_shared, down_shared):
    bf = jnp.bfloat16
    f32 = jnp.float32
    dims = (lax.axis_size("gr"), lax.axis_size("fs"), lax.axis_size("tp"))
    n_gr, n_fs, n_tp = dims
    fs_index = lax.axis_index("fs")
    tp_index = lax.axis_index("tp")
    cols = gate_experts.shape[3]
    per_group = gate_experts.shape[1]
    count = per_group * n_gr
    held = per_group // n_fs
    tok_count, top = routes.shape
    width = tokens.shape[1]

    values = tokens.astype(f32)
    normed = (values * lax.rsqrt(jnp.mean(values * values, axis=-1, keepdims=True) + EPS)).astype(bf)
    named = routes[:, :, None] == jnp.arange(count, dtype=jnp.int32)[None, None, :]
    weight = jnp.sum(jnp.where(named, route_weight[:, :, None], 0.0), axis=1)
    high = lax.reduce_precision(weight, 8, 7)
    extra = -(-2 * count // 128) * 128
    tail = jnp.concatenate(
        [high.astype(bf), (weight - high).astype(bf), jnp.zeros((tok_count, extra - 2 * count), bf)],
        axis=1,
    )
    rows_here = jnp.concatenate([normed, tail], axis=1)

    gain_shared = lax.dynamic_slice_in_dim(
        norm_gain, fs_index * gate_shared.shape[0], gate_shared.shape[0], 0
    )
    shared_here = (
        (gate_shared * gain_shared[:, None]).astype(bf),
        (up_shared * gain_shared[:, None]).astype(bf),
        down_shared.astype(bf),
    )

    gain_cols = lax.dynamic_slice_in_dim(norm_gain, tp_index * cols, cols, 0)
    rows_all, gate_w, up_w = exchange_wide(
        dims,
        rows_here,
        (gate_experts[0] * gain_cols[None, None, :]).astype(bf),
        (up_experts[0] * gain_cols[None, None, :]).astype(bf),
    )

    x = rows_all[:, :width]
    w_all = (
        rows_all[:, width:width + count].astype(f32)
        + rows_all[:, width + count:width + 2 * count].astype(f32)
    )
    units = gate_w.shape[2]
    parts = []
    for g in range(n_gr):
        w_here = lax.dynamic_slice_in_dim(w_all, g * per_group + fs_index * held, held, 1)
        for k in range(held):
            gate = lax.dot_general(x, gate_w[g, k], (((1,), (1,)), ((), ())), preferred_element_type=f32)
            upper = lax.dot_general(x, up_w[g, k], (((1,), (1,)), ((), ())), preferred_element_type=f32)
            parts.append((jax.nn.silu(gate) * upper * w_here[:, k:k + 1]).astype(bf))
    hidden = jnp.stack(parts)
    hidden, down_local, shared_here = lax.optimization_barrier(
        (hidden, down_experts[0].astype(bf), shared_here)
    )
    gate_sw, up_sw, down_sw, down_w = exchange_tall(dims, shared_here, down_local)
    hidden = lax.all_gather(hidden, "tp", axis=0, tiled=False)
    partial = jnp.zeros((), f32)
    down_flat = down_w.reshape(n_gr * held, n_tp, units, cols)
    for i in range(n_gr * held):
        for t in range(n_tp):
            partial = partial + jnp.dot(hidden[t, i], down_flat[i, t], preferred_element_type=f32)
    partial, normed = lax.optimization_barrier((partial.astype(bf), normed))
    routed = lax.psum_scatter(partial, "fs", scatter_dimension=0, tiled=True)

    shared_hidden = (
        jax.nn.silu(jnp.dot(normed, gate_sw, preferred_element_type=f32))
        * jnp.dot(normed, up_sw, preferred_element_type=f32)
    ).astype(bf)
    shared_full = lax.all_gather(shared_hidden, "tp", axis=1, tiled=True)
    shared = jnp.dot(shared_full, down_sw, preferred_element_type=f32)
    mixed = (routed.astype(f32) + shared).astype(bf)
    return (mixed, gate_w, up_w, down_w, gate_sw, up_sw, down_sw)


def solution(mesh):
    return jax.shard_map(
        on_device,
        mesh=mesh,
        in_specs=(
            P(("gr", "fs"), None),
            P(("gr", "fs"), None),
            P(("gr", "fs"), None),
            P(),
            P("gr", None, "fs", "tp"),
            P("gr", None, "fs", "tp"),
            P("gr", None, "fs", "tp"),
            P("fs", "tp"),
            P("fs", "tp"),
            P("fs", "tp"),
        ),
        out_specs=(
            P(("gr", "fs"), "tp"),
            P(None, "fs", "tp", None),
            P(None, "fs", "tp", None),
            P(None, "fs", None, "tp"),
            P(None, "tp"),
            P(None, "tp"),
            P(None, "tp"),
        ),
        check_vma=False,
    )
```

```python
import functools

import jax
import jax.numpy as jnp
from jax import lax
from jax.experimental import pallas as pl
from jax.experimental.pallas import tpu as pltpu
from jax.sharding import PartitionSpec as P

EPS = 1e-06
MESH = pl.DeviceIdType.MESH


def greet_group(dims, gr, fs, tp, barrier):
    n_gr, n_fs, n_tp = dims

    def greet(i, carry):
        f, t = i // n_tp, i % n_tp

        @pl.when((f != fs) | (t != tp))
        def _():
            pl.semaphore_signal(barrier, inc=1, device_id=(gr, f, t), device_id_type=MESH)
        return carry

    lax.fori_loop(0, n_fs * n_tp, greet, 0)
    for p in range(1, n_gr):
        pl.semaphore_signal(
            barrier, inc=1, device_id=((gr + p) % n_gr, fs, tp), device_id_type=MESH
        )
    pl.semaphore_wait(barrier, n_fs * n_tp - 1 + n_gr - 1)


def forward(n_gr, block, s_sem, r_sem, p):
    gr, fs, tp = lax.axis_index("gr"), lax.axis_index("fs"), lax.axis_index("tp")
    return pltpu.make_async_remote_copy(
        src_ref=block, dst_ref=block, send_sem=s_sem, recv_sem=r_sem,
        device_id=((gr + p) % n_gr, fs, tp), device_id_type=MESH,
    )


def wide_steps(dims, g_loc, u_loc, g_out, u_out, send, recv, own, f_send, f_recv):
    n_gr, n_fs, n_tp = dims
    gr, fs, tp = lax.axis_index("gr"), lax.axis_index("fs"), lax.axis_index("tp")
    held = g_loc.shape[0] // n_fs
    rows, cols = g_loc.shape[1], g_loc.shape[2]
    per = g_out.shape[2] // rows
    to_tp = fs // per

    def place(out):
        return out.at[gr, :, pl.ds(pl.multiple_of((fs % per) * rows, rows), rows),
                      pl.ds(pl.multiple_of(tp * cols, cols), cols)]

    def wide(loc, out, m, d):
        k = (fs + d) % n_fs
        return pltpu.make_async_remote_copy(
            src_ref=loc.at[pl.ds(k * held, held)], dst_ref=place(out),
            send_sem=send.at[m, d], recv_sem=recv.at[m, fs % per, tp],
            device_id=(gr, k, to_tp), device_id_type=MESH,
        )

    def wide_own(loc, out, m):
        return pltpu.make_async_copy(loc.at[pl.ds(fs * held, held)], place(out), own.at[m])

    def block(out, g, j, t):
        return out.at[g, :, pl.ds(j * rows, rows), pl.ds(t * cols, cols)]

    pairs = ((g_loc, g_out, 0), (u_loc, u_out, 1))
    for loc, out, m in pairs:
        for d in range(1, n_fs):
            wide(loc, out, m, d).start()

        @pl.when(to_tp == tp)
        def _():
            wide_own(loc, out, m).start()

        @pl.when(to_tp != tp)
        def _():
            wide(loc, out, m, 0).start()
        yield
    for loc, out, m in pairs:
        for j in range(per):
            for t in range(n_tp):
                here = (tp * per + j == fs) & (tp == t)
                part = block(out, gr, j, t)

                @pl.when(here)
                def _():
                    wide_own(loc, out, m).wait()

                @pl.when(jnp.logical_not(here))
                def _():
                    forward(n_gr, part, recv.at[m, j, t], recv.at[m, j, t], 1).wait_recv()
                for p in range(1, n_gr):
                    forward(n_gr, part, f_send.at[m, j, t, p - 1], f_recv.at[m, j, t, p - 1], p).start()
        yield
    for loc, out, m in pairs:
        for d in range(1, n_fs):
            wide(loc, out, m, d).wait_send()

        @pl.when(to_tp != tp)
        def _():
            wide(loc, out, m, 0).wait_send()
        for j in range(per):
            for t in range(n_tp):
                for p in range(1, n_gr):
                    sems = f_send.at[m, j, t, p - 1], f_recv.at[m, j, t, p - 1]
                    forward(n_gr, block(out, gr, j, t), *sems, p).wait_send()
                    forward(n_gr, block(out, (gr + n_gr - p) % n_gr, j, t), *sems, p).wait_recv()


def tall_steps(dims, d_loc, d_out, send, recv, own, f_send, f_recv):
    n_gr, n_fs, n_tp = dims
    gr, fs, tp = lax.axis_index("gr"), lax.axis_index("fs"), lax.axis_index("tp")
    held = d_loc.shape[0] // n_fs
    rows = d_loc.shape[1]

    def block(g, s):
        start = s * rows if isinstance(s, int) else pl.multiple_of(s * rows, rows)
        return d_out.at[g, :, pl.ds(start, rows), :]

    def tall(d):
        k = (fs + d) % n_fs
        return pltpu.make_async_remote_copy(
            src_ref=d_loc.at[pl.ds(k * held, held)], dst_ref=block(gr, fs),
            send_sem=send.at[d], recv_sem=recv.at[fs],
            device_id=(gr, k, tp), device_id_type=MESH,
        )

    mine = pltpu.make_async_copy(d_loc.at[pl.ds(fs * held, held)], block(gr, fs), own)
    for d in range(1, n_fs):
        tall(d).start()
    mine.start()
    yield
    for s in range(n_fs):
        @pl.when(s == fs)
        def _():
            mine.wait()

        @pl.when(s != fs)
        def _():
            forward(n_gr, block(gr, s), recv.at[s], recv.at[s], 1).wait_recv()
        for p in range(1, n_gr):
            forward(n_gr, block(gr, s), f_send.at[s, p - 1], f_recv.at[s, p - 1], p).start()
    yield
    for d in range(1, n_fs):
        tall(d).wait_send()
    for s in range(n_fs):
        for p in range(1, n_gr):
            sems = f_send.at[s, p - 1], f_recv.at[s, p - 1]
            forward(n_gr, block(gr, s), *sems, p).wait_send()
            forward(n_gr, block((gr + n_gr - p) % n_gr, s), *sems, p).wait_recv()


def gather_steps(dims, inner, number, parts, *refs):
    n_gr, n_fs, n_tp = dims
    gr, fs, tp = lax.axis_index("gr"), lax.axis_index("fs"), lax.axis_index("tp")
    ins, outs = refs[:number], refs[number:2 * number]
    z_send, z_recv, y_send, y_recv, x_send, x_recv, own = refs[2 * number:]
    nz = n_fs // inner
    z, y = fs // inner, fs % inner

    def when_next(way, act):
        pl.when(z < nz - 1 if way == 0 else z > 0)(act)

    def beside(way):
        return (gr, (z + 1 if way == 0 else z - 1) * inner + y, tp)

    def block(m, zz, yy):
        rows = ins[m].shape[0]
        return outs[m].at[pl.ds(pl.multiple_of((zz * inner + yy) * rows, rows), rows), :]

    def at(way, d):
        return z - d if way == 0 else z + d

    def z_copy(m, way, d):
        return pltpu.make_async_remote_copy(
            src_ref=ins[m] if d == 0 else block(m, at(way, d), y), dst_ref=block(m, at(way, d), y),
            send_sem=z_send.at[m, way, d], recv_sem=z_recv.at[m, way, d],
            device_id=beside(way), device_id_type=MESH,
        )

    def z_landed(m, way, d):
        part = block(m, at(way, d), y)
        pltpu.make_async_remote_copy(
            src_ref=part, dst_ref=part, send_sem=z_send.at[m, way, d - 1],
            recv_sem=z_recv.at[m, way, d - 1], device_id=beside(way), device_id_type=MESH,
        ).wait_recv()

    def share(m, zz, yy, t):
        rows = ins[m].shape[0]
        sub = rows // parts
        start = (zz * inner + yy) * rows + (t * sub if parts > 1 else 0)
        return outs[m].at[pl.ds(pl.multiple_of(start, sub), sub), :]

    def first_share(m):
        sub = ins[m].shape[0] // parts
        return ins[m].at[pl.ds(pl.multiple_of(tp * sub, sub), sub), :] if parts > 1 else ins[m]

    def y_copy(m, q, way, d, source):
        part = share(m, at(way, d), source, tp)
        i = d + way * (nz - 1) if d else 0
        return pltpu.make_async_remote_copy(
            src_ref=first_share(m) if d == 0 else part, dst_ref=part,
            send_sem=y_send.at[m, q - 1, i], recv_sem=y_recv.at[m, q - 1, i],
            device_id=(gr, z * inner + (y + q) % inner, tp), device_id_type=MESH,
        )

    def x_copy(m, q, way, d, r, holder):
        part = share(m, at(way, d), (y + inner - q) % inner, holder)
        i = d + way * (nz - 1) if d else 0
        return pltpu.make_async_remote_copy(
            src_ref=part, dst_ref=part,
            send_sem=x_send.at[m, q - 1, i, r - 1], recv_sem=x_recv.at[m, q - 1, i, r - 1],
            device_id=(gr, fs, (tp + r) % n_tp), device_id_type=MESH,
        )

    def hand_over(distance):
        for d, way in places:
            if d != distance:
                continue

            def act(d=d, way=way):
                for m in range(number):
                    for q in range(1, inner):
                        y_copy(m, q, way, d, (y + inner - q) % inner).wait_recv()
                        for r in range(1, parts):
                            x_copy(m, q, way, d, r, tp).start()
            steps(d, way, act)

    def own_copy(m):
        return pltpu.make_async_copy(ins[m], block(m, z, y), own.at[m])

    def steps(d, way, act):
        if d == 0:
            act()
        else:
            pl.when(z - d >= 0 if way == 0 else z + d < nz)(act)

    places = [(0, 0)] + [(d, way) for d in range(1, nz) for way in (0, 1)]
    for m in range(number):
        for way in (0, 1):
            when_next(way, lambda m=m, way=way: z_copy(m, way, 0).start())
        for q in range(1, inner):
            y_copy(m, q, 0, 0, y).start()
    for m in range(number):
        own_copy(m).start()
    yield
    for d, way in places[1:]:
        def pass_on(d=d, way=way):
            for m in range(number):
                z_landed(m, way, d)
                if d < nz - 1:
                    when_next(way, lambda: z_copy(m, way, d).start())
                for q in range(1, inner):
                    y_copy(m, q, way, d, y).start()
        steps(d, way, pass_on)
        if way:
            hand_over(d - 1)
            yield
    hand_over(nz - 1)
    for m in range(number):
        for way in (0, 1):
            when_next(way, lambda m=m, way=way: z_copy(m, way, 0).wait_send())
    for d, way in places:
        def finish(d=d, way=way):
            for m in range(number):
                if 0 < d < nz - 1:
                    when_next(way, lambda: z_copy(m, way, d).wait_send())
                for q in range(1, inner):
                    y_copy(m, q, way, d, y).wait_send()
                    for r in range(1, parts):
                        x_copy(m, q, way, d, r, tp).wait_send()
                        x_copy(m, q, way, d, r, (tp + n_tp - r) % n_tp).wait_recv()
        steps(d, way, finish)
    for m in range(number):
        own_copy(m).wait()


def run_steps(first, second):
    live = [first, second]
    while live:
        for steps in list(live):
            if next(steps, live) is live:
                live.remove(steps)


def fused_kernel(dims, inner, number, parts, main_steps, main_ins, main_outs, main_sems, *refs):
    gr, fs, tp = lax.axis_index("gr"), lax.axis_index("fs"), lax.axis_index("tp")
    greet_group(dims, gr, fs, tp, pltpu.get_barrier_semaphore())
    edges = [0]
    for n in (number, main_ins, number, main_outs, 7, main_sems):
        edges.append(edges[-1] + n)
    a, b, c, d, e, f = [refs[edges[i]:edges[i + 1]] for i in range(6)]
    run_steps(gather_steps(dims, inner, number, parts, *a, *c, *e), main_steps(dims, *b, *d, *f))


def exchange(dims, ident, work, main_steps, same_on_tp, arrays, main_args, main_outs, main_sems):
    n_fs = dims[1]
    inner = 2 if n_fs % 2 == 0 else 1
    nz = n_fs // inner
    number = len(arrays)
    outs = tuple(jax.ShapeDtypeStruct((n_fs * a.shape[0], a.shape[1]), a.dtype) for a in arrays)
    chain = (number, 2, max(1, nz - 1))
    across = (number, max(1, inner - 1), 2 * nz - 1)
    n_tp = dims[2]
    parts = n_tp if same_on_tp and all(a.shape[0] % (8 * n_tp) == 0 for a in arrays) else 1
    over = (*across, max(1, parts - 1))
    sems = [chain, chain, across, across, over, over, (number,), *main_sems]
    args = (*arrays, *main_args)
    outs = outs + tuple(main_outs)
    return pl.pallas_call(
        functools.partial(
            fused_kernel, dims, inner, number, parts, main_steps,
            len(main_args), len(main_outs), len(main_sems),
        ),
        out_shape=outs,
        in_specs=[pl.BlockSpec(memory_space=pl.ANY)] * len(args),
        out_specs=tuple(pl.BlockSpec(memory_space=pl.ANY) for _ in outs),
        scratch_shapes=[pltpu.SemaphoreType.DMA(shape) for shape in sems],
        compiler_params=pltpu.CompilerParams(collective_id=ident, has_side_effects=True),
        cost_estimate=pl.CostEstimate(flops=0, bytes_accessed=work, transcendentals=0),
    )(*args)


def exchange_wide(dims, rows_here, g_loc, u_loc):
    n_gr, n_fs, n_tp = dims
    count, rows, cols = g_loc.shape
    per = n_fs // n_tp
    out = jax.ShapeDtypeStruct((n_gr, count // n_fs, per * rows, n_tp * cols), g_loc.dtype)
    halves = (2, per, n_tp, n_gr - 1)
    return exchange(
        dims, 1, 200 << 20, wide_steps, True, (rows_here,), (g_loc, u_loc), (out, out),
        [(2, n_fs), (2, per, n_tp), (2,), halves, halves],
    )


def exchange_tall(dims, shared_here, d_loc):
    n_gr, n_fs, n_tp = dims
    count, rows, cols = d_loc.shape
    out = jax.ShapeDtypeStruct((n_gr, count // n_fs, n_fs * rows, cols), d_loc.dtype)
    return exchange(
        dims, 2, 100 << 20, tall_steps, False, shared_here, (d_loc,), (out,),
        [(n_fs,), (n_fs,), (), (n_fs, n_gr - 1), (n_fs, n_gr - 1)],
    )


def on_device(tokens, routes, route_weight, norm_gain, gate_experts, up_experts, down_experts,
              gate_shared, up_shared, down_shared):
    bf = jnp.bfloat16
    f32 = jnp.float32
    dims = (lax.axis_size("gr"), lax.axis_size("fs"), lax.axis_size("tp"))
    n_gr, n_fs, n_tp = dims
    fs_index = lax.axis_index("fs")
    tp_index = lax.axis_index("tp")
    cols = gate_experts.shape[3]
    per_group = gate_experts.shape[1]
    count = per_group * n_gr
    held = per_group // n_fs
    tok_count, top = routes.shape
    width = tokens.shape[1]

    values = tokens.astype(f32)
    normed = (values * lax.rsqrt(jnp.mean(values * values, axis=-1, keepdims=True) + EPS)).astype(bf)
    named = routes[:, :, None] == jnp.arange(count, dtype=jnp.int32)[None, None, :]
    weight = jnp.sum(jnp.where(named, route_weight[:, :, None], 0.0), axis=1)
    high = lax.reduce_precision(weight, 8, 7)
    extra = -(-2 * count // 128) * 128
    tail = jnp.concatenate(
        [high.astype(bf), (weight - high).astype(bf), jnp.zeros((tok_count, extra - 2 * count), bf)],
        axis=1,
    )
    rows_here = jnp.concatenate([normed, tail], axis=1)

    gain_shared = lax.dynamic_slice_in_dim(
        norm_gain, fs_index * gate_shared.shape[0], gate_shared.shape[0], 0
    )
    shared_here = (
        (gate_shared * gain_shared[:, None]).astype(bf),
        (up_shared * gain_shared[:, None]).astype(bf),
        down_shared.astype(bf),
    )

    gain_cols = lax.dynamic_slice_in_dim(norm_gain, tp_index * cols, cols, 0)
    rows_all, gate_w, up_w = exchange_wide(
        dims,
        rows_here,
        (gate_experts[0] * gain_cols[None, None, :]).astype(bf),
        (up_experts[0] * gain_cols[None, None, :]).astype(bf),
    )

    x = rows_all[:, :width]
    w_all = (
        rows_all[:, width:width + count].astype(f32)
        + rows_all[:, width + count:width + 2 * count].astype(f32)
    )
    units = gate_w.shape[2]
    parts = []
    for g in range(n_gr):
        w_here = lax.dynamic_slice_in_dim(w_all, g * per_group + fs_index * held, held, 1)
        for k in range(held):
            gate = lax.dot_general(x, gate_w[g, k], (((1,), (1,)), ((), ())), preferred_element_type=f32)
            upper = lax.dot_general(x, up_w[g, k], (((1,), (1,)), ((), ())), preferred_element_type=f32)
            parts.append((jax.nn.silu(gate) * upper * w_here[:, k:k + 1]).astype(bf))
    hidden = jnp.stack(parts)
    hidden, down_local, shared_here = lax.optimization_barrier(
        (hidden, down_experts[0].astype(bf), shared_here)
    )
    gate_sw, up_sw, down_sw, down_w = exchange_tall(dims, shared_here, down_local)
    hidden = lax.all_gather(hidden, "tp", axis=0, tiled=False)
    partial = jnp.zeros((), f32)
    down_flat = down_w.reshape(n_gr * held, n_tp, units, cols)
    for i in range(n_gr * held):
        for t in range(n_tp):
            partial = partial + jnp.dot(hidden[t, i], down_flat[i, t], preferred_element_type=f32)
    partial, normed = lax.optimization_barrier((partial.astype(bf), normed))
    routed = lax.psum_scatter(partial, "fs", scatter_dimension=0, tiled=True)

    shared_hidden = (
        jax.nn.silu(jnp.dot(normed, gate_sw, preferred_element_type=f32))
        * jnp.dot(normed, up_sw, preferred_element_type=f32)
    ).astype(bf)
    shared_full = lax.all_gather(shared_hidden, "tp", axis=1, tiled=True)
    shared = jnp.dot(shared_full, down_sw, preferred_element_type=f32)
    mixed = (routed.astype(f32) + shared).astype(bf)
    return (mixed, gate_w, up_w, down_w, gate_sw, up_sw, down_sw)


def solution(mesh):
    return jax.shard_map(
        on_device,
        mesh=mesh,
        in_specs=(
            P(("gr", "fs"), None),
            P(("gr", "fs"), None),
            P(("gr", "fs"), None),
            P(),
            P("gr", None, "fs", "tp"),
            P("gr", None, "fs", "tp"),
            P("gr", None, "fs", "tp"),
            P("fs", "tp"),
            P("fs", "tp"),
            P("fs", "tp"),
        ),
        out_specs=(
            P(("gr", "fs"), "tp"),
            P(None, "fs", "tp", None),
            P(None, "fs", "tp", None),
            P(None, "fs", None, "tp"),
            P(None, "tp"),
            P(None, "tp"),
            P(None, "tp"),
        ),
        check_vma=False,
    )
```
